32 devices in a mesh: sp: 8 (over z, y), tp: 4 (over x, core).
Axes of the slice: x: 2, y: 2, z: 4, core: 2. Of those that a mesh axis runs over, the one named last changes fastest.
Arguments:
- skip_stream: bfloat16 [6144, 2048], P(('sp', 'tp')), may hold values from -24 to 24
- acceptance_signal: bfloat16 [6144, 2048], P('sp', 'tp'), may hold values from -6 to 6
- lookup_mapped: bfloat16 [6144, 2048], P('sp', 'tp'), may hold values from -12 to 12
- payload_mapped: bfloat16 [6144, 2048], P('sp', 'tp'), may hold values from -6 to 6
- result_switch: bfloat16 [6144, 2048], P('sp', 'tp'), may hold values from -6 to 6
- forget_dynamic_share: bfloat16 [6144, 2048], P('sp', 'tp'), may hold values from -4 to 4
- additive_forget_logarithm: float32 [6144, 32], P('sp', 'tp'), may hold values from -1 to 0
- forget_feature_offset: float32 [2048], P('tp'), may hold values from -11 to -3
- substitution_dynamic_share: bfloat16 [6144, 2048], P('sp', 'tp'), may hold values from -6 to 6
- substitution_feature_offset: float32 [2048], P('tp'), may hold values from -6.5 to 2.5
- diagonal_reward_scales: float32 [2048], P('tp'), may hold values from -0.9 to 0.9
- result_matrix: bfloat16 [2048, 2048], P('tp'), may hold values from -0.125 to 0.125
- mlp_rescaler: float32 [2048], replicated, may hold values from 0.1 to 1.9
- switch_matrix: bfloat16 [2048, 5120], P('sp', 'tp'), may hold values from -0.125 to 0.125
- expand_matrix: bfloat16 [2048, 5120], P('sp', 'tp'), may hold values from -0.125 to 0.125
- contract_matrix: bfloat16 [2048, 5120], P('sp', 'tp'), may hold values from -0.25 to 0.25
Outputs:
- mixed_out: bfloat16 [6144, 2048], P(('sp', 'tp'))
The draws below stay inside these ranges and needn't reach their ends.
All inputs are finite; a program needn't handle non-finite values.
Results may differ from the reference program's by a relative error of at most 0.015.
Values may be sent and summed in bfloat16 or wider, within the bound.
A program may use at most 128 MiB of HBM per device.

```python
import jax
import jax.numpy as jnp
from jax import lax

EMBED_DIMENSION = 2048
PER_GROUP_DIMS = 64
FF = 5120
TOK_DEV = 768
TOKENS = 6144
N_TP = 4


def draw_skip_stream(key, part):
    entries = jnp.clip(jax.random.normal(jax.random.fold_in(key, 11), (TOKENS, EMBED_DIMENSION), jnp.float32), -4.0, 4.0)
    column_scale = jnp.exp(jnp.linspace(jnp.log(0.3), jnp.log(3.0), EMBED_DIMENSION))
    row_scale = jnp.exp(jax.random.uniform(jax.random.fold_in(key, 12), (TOKENS, 1), jnp.float32, jnp.log(0.5), jnp.log(2.0)))
    return (entries * column_scale[None, :] * row_scale).astype(jnp.bfloat16)


def draw_lookup_mapped(key, part):
    attention_groups = EMBED_DIMENSION // PER_GROUP_DIMS
    direction = jnp.clip(jax.random.normal(jax.random.fold_in(key, 51), (attention_groups, PER_GROUP_DIMS), jnp.float32), -4.0, 4.0)
    noise = jnp.clip(jax.random.normal(jax.random.fold_in(key, 52), (TOKENS, attention_groups, PER_GROUP_DIMS), jnp.float32), -4.0, 4.0)
    weight = 2.0 * jnp.ones((attention_groups, 1), jnp.float32)
    shared = weight * direction
    return (noise + shared[None, :, :]).reshape(TOKENS, EMBED_DIMENSION).astype(jnp.bfloat16)


def draw_forget_dynamic_share(key, part):
    blocks = TOKENS // TOK_DEV
    offset = jax.random.uniform(jax.random.fold_in(key, 21), (blocks, 1, 1), jnp.float32, -0.7, 0.7)
    noise = jnp.clip(jax.random.normal(jax.random.fold_in(key, 22), (blocks, TOK_DEV, EMBED_DIMENSION), jnp.float32), -3.0, 3.0)
    return (noise + offset).reshape(TOKENS, EMBED_DIMENSION).astype(jnp.bfloat16)


def draw_additive_forget_logarithm(key, part):
    spots = jax.random.randint(jax.random.fold_in(key, 31), (4,), 0, TOKENS)
    struck = jnp.any(jnp.arange(TOKENS)[:, None] == spots[None, :], axis=1)
    losses = jnp.log(jax.random.uniform(jax.random.fold_in(key, 32), (TOKENS, EMBED_DIMENSION // PER_GROUP_DIMS), jnp.float32, 0.5, 0.8))
    return jnp.where(struck[:, None], losses, 0.0).astype(jnp.float32)


def draw_forget_feature_offset(key, part):
    attention_groups = EMBED_DIMENSION // PER_GROUP_DIMS
    fast_share = 0.5
    quick_heads = jax.random.uniform(jax.random.fold_in(key, 41), (attention_groups, 1), jnp.float32) < fast_share
    quick = jax.random.uniform(jax.random.fold_in(key, 42), (attention_groups, PER_GROUP_DIMS), jnp.float32, -4.5, -3.0)
    patient = jax.random.uniform(jax.random.fold_in(key, 43), (attention_groups, PER_GROUP_DIMS), jnp.float32, -11.0, -9.0)
    return jnp.where(quick_heads, quick, patient).reshape(EMBED_DIMENSION).astype(jnp.float32)


def draw_substitution_feature_offset(key, part):
    attention_groups = EMBED_DIMENSION // PER_GROUP_DIMS
    order = jax.random.permutation(jax.random.fold_in(key, 61), attention_groups)
    levels = jnp.linspace(-6.0, 2.2, attention_groups)
    jitter = jax.random.uniform(jax.random.fold_in(key, 62), (attention_groups, PER_GROUP_DIMS), jnp.float32, -0.3, 0.3)
    return (levels[order][:, None] + jitter).reshape(EMBED_DIMENSION).astype(jnp.float32)


def steps_of(key, dims, split, least, top_value):
    gain = 1.0
    for dim, shards_of in split:
        steps = jax.random.uniform(jax.random.fold_in(jax.random.fold_in(key, 6), dim), (shards_of,), jnp.float32, least / len(split), top_value / len(split))
        gain = gain * jnp.repeat(jnp.exp(steps), dims[dim] // shards_of).reshape((-1,) + (1,) * (len(dims) - 1 - dim))
    return gain


def scatter_about(key, dims, scale, limit, cuts=(), kind=jnp.bfloat16):
    values = scale * jax.random.normal(key, dims, jnp.float32)
    if cuts:
        values = values * steps_of(key, dims, cuts, -0.22, 0.18)
    return jnp.clip(values, -limit, limit).astype(kind)


def setup_inputs(seed: int = 0) -> dict:
    seeds = jax.random.split(jax.random.key(seed), 17)
    skip_stream = draw_skip_stream(jax.random.fold_in(seeds[16], 71), 0)
    acceptance_signal = scatter_about(seeds[1], (TOKENS, EMBED_DIMENSION), 1.0, 6.0, ((0, 8), (1, 4)))
    lookup_mapped = draw_lookup_mapped(jax.random.fold_in(seeds[16], 71), 0)
    payload_mapped = scatter_about(seeds[3], (TOKENS, EMBED_DIMENSION), 1.0, 6.0, ((0, 8), (1, 4)))
    result_switch = scatter_about(seeds[4], (TOKENS, EMBED_DIMENSION), 1.0, 6.0, ((0, 8), (1, 4)))
    forget_dynamic_share = draw_forget_dynamic_share(jax.random.fold_in(seeds[16], 71), 0)
    additive_forget_logarithm = draw_additive_forget_logarithm(jax.random.fold_in(seeds[16], 71), 0)
    forget_feature_offset = draw_forget_feature_offset(jax.random.fold_in(seeds[16], 71), 0)
    substitution_dynamic_share = scatter_about(seeds[8], (TOKENS, EMBED_DIMENSION), 1.0, 6.0, ((0, 8), (1, 4)))
    substitution_feature_offset = draw_substitution_feature_offset(jax.random.fold_in(seeds[16], 71), 0)
    diagonal_reward_scales = scatter_about(seeds[10], (EMBED_DIMENSION,), 0.15, 0.9, ((0, 4),), jnp.float32)
    result_matrix = scatter_about(seeds[11], (EMBED_DIMENSION, EMBED_DIMENSION), EMBED_DIMENSION ** -0.5, 0.125, ((0, 4),))
    mlp_rescaler = jnp.clip(1.0 + 0.18 * jax.random.normal(seeds[12], (EMBED_DIMENSION,), jnp.float32), 0.1, 1.9)
    switch_matrix = scatter_about(seeds[13], (EMBED_DIMENSION, FF), EMBED_DIMENSION ** -0.5, 0.125, ((0, 8), (1, 4)))
    expand_matrix = scatter_about(seeds[14], (EMBED_DIMENSION, FF), EMBED_DIMENSION ** -0.5, 0.125, ((0, 8), (1, 4)))
    contract_matrix = scatter_about(seeds[15], (EMBED_DIMENSION, FF), (FF // 8) ** -0.5, 0.25, ((0, 8), (1, 4)))
    return dict(skip_stream=skip_stream, acceptance_signal=acceptance_signal, lookup_mapped=lookup_mapped, payload_mapped=payload_mapped, result_switch=result_switch, forget_dynamic_share=forget_dynamic_share, additive_forget_logarithm=additive_forget_logarithm, forget_feature_offset=forget_feature_offset, substitution_dynamic_share=substitution_dynamic_share, substitution_feature_offset=substitution_feature_offset, diagonal_reward_scales=diagonal_reward_scales, result_matrix=result_matrix, mlp_rescaler=mlp_rescaler, switch_matrix=switch_matrix, expand_matrix=expand_matrix, contract_matrix=contract_matrix)


norm_eps = 1e-06
group_eps = 0.00064
half_step = 0.5

def group_sum(left, right, groups):
    span = left.shape[1] // groups

    def add_group(total, index):
        first = (index * span).astype(jnp.int32)
        left_part = lax.dynamic_slice_in_dim(left, first, span, 1)
        right_part = lax.dynamic_slice_in_dim(right, first, span, 0)
        partial_prod = jnp.dot(left_part, right_part, preferred_element_type=jnp.float32)
        partial_prod = lax.optimization_barrier(partial_prod.astype(jnp.bfloat16)).astype(jnp.float32)
        return (total + partial_prod, None)
    start_total = jnp.zeros((left.shape[0], right.shape[1]), jnp.float32)
    total, _ = lax.scan(add_group, start_total, jnp.arange(groups, dtype=jnp.int32))
    return total.astype(jnp.bfloat16)

def advance(memory, inputs):
    read_now, decay_now, key_now, value_now, unit_now, rate_now = inputs
    recall = lax.optimization_barrier(jnp.sum(memory * unit_now[:, None, :], axis=-1))
    memory = memory * decay_now[:, None, :] - recall[:, :, None] * (unit_now * rate_now)[:, None, :] + value_now[:, :, None] * key_now[:, None, :]
    return (memory, lax.optimization_barrier(jnp.sum(memory * read_now[:, None, :], axis=-1)))

def reference(skip_stream, acceptance_signal, lookup_mapped, payload_mapped, result_switch, forget_dynamic_share, additive_forget_logarithm, forget_feature_offset, substitution_dynamic_share, substitution_feature_offset, diagonal_reward_scales, result_matrix, mlp_rescaler, switch_matrix, expand_matrix, contract_matrix):
    sequence_span = skip_stream.shape[0]
    attention_groups = EMBED_DIMENSION // PER_GROUP_DIMS

    def by_head(values):
        return values.astype(jnp.float32).reshape(sequence_span, attention_groups, PER_GROUP_DIMS)
    acceptance_lines = by_head(acceptance_signal)
    lookup_vectors = by_head(lookup_mapped)
    payload_vectors = by_head(payload_mapped)
    log_decay_rate = -jax.nn.softplus(-(forget_feature_offset[None, :] + forget_dynamic_share.astype(jnp.float32))) - 0.5
    decay_factor_step = jnp.exp(-jnp.exp(log_decay_rate).reshape(sequence_span, attention_groups, PER_GROUP_DIMS) + additive_forget_logarithm[:, :, None])
    replace_rate = jax.nn.sigmoid(substitution_feature_offset[None, :] + substitution_dynamic_share.astype(jnp.float32))
    replace_rate = replace_rate.reshape(sequence_span, attention_groups, PER_GROUP_DIMS)
    unit_key = lookup_vectors * lax.rsqrt(lax.optimization_barrier(jnp.sum(lookup_vectors * lookup_vectors, axis=-1, keepdims=True)) + norm_eps)
    start_memory = jnp.zeros((attention_groups, PER_GROUP_DIMS, PER_GROUP_DIMS), jnp.float32)
    _, outcome = lax.scan(advance, start_memory, (acceptance_lines, decay_factor_step, lookup_vectors, payload_vectors, unit_key, replace_rate))
    centre = lax.optimization_barrier(jnp.mean(outcome, axis=-1, keepdims=True))
    spread = lax.optimization_barrier(jnp.mean(jnp.square(outcome - centre), axis=-1, keepdims=True))
    rescaled_attention = (outcome - centre) * lax.rsqrt(spread + group_eps)
    diagonal_reward_summand = lax.optimization_barrier(jnp.sum(acceptance_lines * lookup_vectors * diagonal_reward_scales.reshape(attention_groups, PER_GROUP_DIMS), axis=-1, keepdims=True)) * payload_vectors
    merged_attention = ((rescaled_attention + diagonal_reward_summand).reshape(sequence_span, EMBED_DIMENSION) * result_switch.astype(jnp.float32)).astype(jnp.bfloat16)
    projected = group_sum(merged_attention, result_matrix, N_TP)
    stream = skip_stream.astype(jnp.float32) + projected.astype(jnp.float32)
    scale_rows = lax.rsqrt(lax.optimization_barrier(jnp.mean(stream * stream, axis=-1, keepdims=True)) + norm_eps)
    normed_rows = (stream * scale_rows * mlp_rescaler[None, :]).astype(jnp.bfloat16)
    gate_act = jnp.dot(normed_rows, switch_matrix, preferred_element_type=jnp.float32)
    up_act = jnp.dot(normed_rows, expand_matrix, preferred_element_type=jnp.float32)
    hidden = (jax.nn.silu(gate_act) * up_act).astype(jnp.bfloat16)
    ffn_out = group_sum(hidden, contract_matrix.T, N_TP)
    return (stream + half_step * ffn_out.astype(jnp.float32)).astype(jnp.bfloat16)
```

```python
import functools

import jax
import jax.numpy as jnp
from jax import lax
from jax.experimental import pallas as pl
from jax.experimental.pallas import tpu as pltpu
from jax.sharding import PartitionSpec as P

PER_GROUP_DIMS = 64


norm_eps = 1e-06
group_eps = 0.00064
half_step = 0.5
exact = lax.Precision.HIGHEST

PAIR = 2 * PER_GROUP_DIMS
CHUNK = 64
ROWS_OUT = 256
NT = (((1,), (1,)), ((), ()))
NN = (((1,), (0,)), ((), ()))
TN = (((0,), (0,)), ((), ()))
bf16 = jnp.bfloat16
f32 = jnp.float32
P_SCORE, P_INV, P_SOLVE, P_OUT, P_STATE = 3, 1, 3, 3, 1


def mm(left, right, dims, passes):
    if passes == 6:
        return lax.dot_general(left, right, dims, precision=exact, preferred_element_type=f32)
    left_hi, right_hi = left.astype(bf16), right.astype(bf16)
    total = lax.dot_general(left_hi, right_hi, dims, preferred_element_type=f32)
    if passes == 3:
        left_lo = (left - left_hi.astype(f32)).astype(bf16)
        right_lo = (right - right_hi.astype(f32)).astype(bf16)
        total += lax.dot_general(left_hi, right_lo, dims, preferred_element_type=f32)
        total += lax.dot_general(left_lo, right_hi, dims, preferred_element_type=f32)
    return total


def halves(shape):
    return lax.broadcasted_iota(jnp.int32, shape, 1) < PER_GROUP_DIMS


def stack(values):
    first = halves(values.shape)
    zero = jnp.zeros_like(values)
    return jnp.concatenate([jnp.where(first, values, zero), jnp.where(first, zero, values)], 0)


def fold(values):
    size = values.shape[0] // 2
    return values[:size] + values[size:]


def head_sums(values):
    row = lax.broadcasted_iota(jnp.int32, (PAIR, PAIR), 0) // PER_GROUP_DIMS
    col = lax.broadcasted_iota(jnp.int32, (PAIR, PAIR), 1) // PER_GROUP_DIMS
    ones = jnp.where(row == col, 1.0, 0.0).astype(bf16)
    hi = values.astype(bf16)
    left = values - hi.astype(f32)
    mid = left.astype(bf16)
    low = (left - mid.astype(f32)).astype(bf16)
    return (
        jnp.dot(hi, ones, preferred_element_type=f32)
        + jnp.dot(mid, ones, preferred_element_type=f32)
        + jnp.dot(low, ones, preferred_element_type=f32)
    )


def recur_kernel(
    read_ref, key_ref, value_ref, forget_ref, added_ref, rate_ref, forget_off_ref, rate_off_ref,
    out_ref, coef_ref, state_out_ref, map_out_ref, memory,
):
    pairs = read_ref.shape[1] // PAIR
    span = range(pairs)
    row = lax.broadcasted_iota(jnp.int32, (PAIR, PAIR), 0)
    col = lax.broadcasted_iota(jnp.int32, (PAIR, PAIR), 1)
    diagonal = jnp.where(row == col, 1.0, 0.0)
    same_head = (row // CHUNK) == (col // CHUNK)
    strict = same_head & (col < row)
    inclusive = same_head & (col <= row)

    @pl.when(pl.program_id(0) == 0)
    def _():
        for p in span:
            memory[p, :PAIR] = jnp.zeros((PAIR, PAIR), f32)
            memory[p, PAIR:] = diagonal

    lower = (
        lax.broadcasted_iota(jnp.int32, (CHUNK, CHUNK), 1)
        <= lax.broadcasted_iota(jnp.int32, (CHUNK, CHUNK), 0)
    )
    lower = jnp.where(lower, 1.0, 0.0)
    first = halves((CHUNK, PAIR))
    at = [slice(p * PAIR, (p + 1) * PAIR) for p in span]
    decay_rate = [
        jax.nn.sigmoid(forget_off_ref[:, at[p]] + forget_ref[:, at[p]].astype(f32)) for p in span
    ]
    log_step = [
        -0.6065306597126334 * decay_rate[p]
        + jnp.where(first, added_ref[:, 2 * p : 2 * p + 1], added_ref[:, 2 * p + 1 : 2 * p + 2])
        for p in span
    ]
    cumulate = [mm(lower, log_step[p], NN, 6) for p in span]
    key = [key_ref[:, at[p]].astype(f32) for p in span]
    unit = [key[p] * lax.rsqrt(head_sums(key[p] * key[p]) + norm_eps) for p in span]
    erase = [
        unit[p] * jax.nn.sigmoid(rate_off_ref[:, at[p]] + rate_ref[:, at[p]].astype(f32))
        for p in span
    ]
    middle = [cumulate[p][CHUNK // 2 - 1 : CHUNK // 2] for p in span]
    last = [cumulate[p][CHUNK - 1 : CHUNK] for p in span]
    growth = [jnp.exp(cumulate[p] - middle[p]) for p in span]
    shrink = [jnp.exp(middle[p] - cumulate[p]) for p in span]
    to_middle = [jnp.exp(middle[p]) for p in span]
    from_middle = [jnp.exp(last[p] - middle[p]) for p in span]
    over_chunk = [jnp.exp(last[p]) for p in span]
    before = [jnp.exp(cumulate[p] - log_step[p] - middle[p]) * unit[p] for p in span]
    read = [read_ref[:, at[p]].astype(f32) * growth[p] for p in span]
    key_back = [key[p] * shrink[p] for p in span]
    erase_back = [erase[p] * shrink[p] for p in span]
    score = [
        mm(
            jnp.concatenate([stack(before[p]), stack(read[p])], 0),
            jnp.concatenate([stack(key_back[p]), stack(erase_back[p])], 0),
            NT,
            P_SCORE,
        )
        for p in span
    ]
    key_past = [jnp.where(strict, score[p][:PAIR, :PAIR], 0.0) for p in span]
    erase_past = [jnp.where(strict, score[p][:PAIR, PAIR:], 0.0) for p in span]
    key_read = [jnp.where(inclusive, score[p][PAIR:, :PAIR], 0.0) for p in span]
    erase_read = [jnp.where(inclusive, score[p][PAIR:, PAIR:], 0.0) for p in span]
    value = [stack(value_ref[:, at[p]]).astype(f32) for p in span]
    recall = [mm(key_past[p], value[p], NN, P_SOLVE) for p in span]
    inverse = [
        diagonal - jnp.where((row // 2) == (col // 2), erase_past[p], 0.0) for p in span
    ]
    size = 2
    while size < CHUNK:
        off = ((row // (2 * size)) == (col // (2 * size))) & ((row // size) != (col // size))
        part = [mm(jnp.where(off, erase_past[p], 0.0), inverse[p], NN, P_INV) for p in span]
        inverse = [inverse[p] - mm(inverse[p], part[p], NN, P_INV) for p in span]
        size *= 2
    solved = [
        mm(
            inverse[p],
            jnp.concatenate([recall[p], stack(before[p] * to_middle[p])], 1),
            NN,
            P_SOLVE,
        )
        for p in span
    ]
    inner = [
        mm(
            jnp.concatenate([key_read[p], -erase_read[p]], 1),
            jnp.concatenate(
                [jnp.concatenate([value[p], jnp.zeros_like(value[p])], 1), solved[p]], 0
            ),
            NN,
            P_OUT,
        )
        for p in span
    ]
    local = [fold(inner[p][:, :PAIR]) for p in span]
    from_start = [fold(inner[p][:, PAIR:]) + read[p] * to_middle[p] for p in span]
    both = [memory[p] for p in span]
    passed = [mm(from_start[p], both[p], NT, P_STATE) for p in span]
    for p in span:
        out_ref[:, at[p]] = local[p] + passed[p][:, :PAIR]
        coef_ref[:, at[p]] = passed[p][:, PAIR:].astype(bf16)
    key_end = [key_back[p] * from_middle[p] for p in span]
    erase_end = [erase_back[p] * from_middle[p] for p in span]
    recalled = [fold(solved[p][:, :PAIR]) for p in span]
    carried_map = [fold(solved[p][:, PAIR:]) for p in span]
    added = [
        mm(
            jnp.concatenate([value_ref[:, at[p]].astype(f32), -recalled[p]], 0),
            jnp.concatenate([key_end[p], erase_end[p]], 0),
            TN,
            P_OUT,
        )
        for p in span
    ]
    step_map = [mm(carried_map[p], erase_end[p], TN, P_OUT) for p in span]
    for p in span:
        moved = mm(both[p], jnp.where(same_head, step_map[p], 0.0), NN, P_STATE)
        kept = both[p] * over_chunk[p] - moved
        memory[p, :PAIR] = kept[:PAIR] + jnp.where(same_head, added[p], 0.0)
        memory[p, PAIR:] = kept[PAIR:]

    @pl.when(pl.program_id(0) == pl.num_programs(0) - 1)
    def _():
        for p in span:
            state_out_ref[p] = fold(memory[p, :PAIR]).astype(bf16)
            map_out_ref[p] = fold(memory[p, PAIR:]).astype(bf16)


def recurrence(read, key, value, forget, added, rate, forget_off, rate_off):
    length, breadth = read.shape
    pairs = breadth // PAIR
    wide = pl.BlockSpec((CHUNK, breadth), lambda c: (c, 0))
    vector = pl.BlockSpec((1, breadth), lambda c: (0, 0))
    closing = pl.BlockSpec((pairs, PER_GROUP_DIMS, PAIR), lambda c: (0, 0, 0))
    closing_shape = jax.ShapeDtypeStruct((pairs, PER_GROUP_DIMS, PAIR), bf16)
    return pl.pallas_call(
        recur_kernel,
        grid=(length // CHUNK,),
        in_specs=[
            wide, wide, wide, wide,
            pl.BlockSpec((CHUNK, added.shape[1]), lambda c: (c, 0)),
            wide, vector, vector,
        ],
        out_specs=[wide, wide, closing, closing],
        out_shape=[
            jax.ShapeDtypeStruct((length, breadth), f32),
            jax.ShapeDtypeStruct((length, breadth), bf16),
            closing_shape,
            closing_shape,
        ],
        scratch_shapes=[pltpu.VMEM((pairs, 2 * PAIR, PAIR), f32)],
        cost_estimate=pl.CostEstimate(
            flops=length * breadth * 200000, bytes_accessed=length * breadth * 16, transcendentals=0
        ),
        name="recurrence",
    )(read, key, value, forget, added, rate, forget_off[None, :], rate_off[None, :])


def merge_kernel(
    place_ref, local_ref, coef_ref, states_ref, maps_ref, read_ref, key_ref, value_ref,
    switch_ref, scales_ref, matrix_ref, out_ref, carried, merged,
):
    pairs = local_ref.shape[1] // PAIR
    span = range(pairs)

    @pl.when(pl.program_id(0) == 0)
    def _():
        for p in span:
            carried[p] = jnp.zeros((PAIR, PAIR), f32)

        def one(turn, _):
            for p in span:
                carried[p] = mm(
                    carried[p], stack(maps_ref[turn, p].astype(f32)), NN, 3
                ) + stack(states_ref[turn, p].astype(f32))
            return 0

        lax.fori_loop(0, place_ref[0], one, 0)

    for p in span:
        at = slice(p * PAIR, (p + 1) * PAIR)
        outcome = local_ref[:, at] + mm(coef_ref[:, at].astype(f32), carried[p], NT, 1)
        centred = outcome - head_sums(outcome) * (1.0 / PER_GROUP_DIMS)
        spread = head_sums(centred * centred) * (1.0 / PER_GROUP_DIMS)
        normed = centred * lax.rsqrt(spread + group_eps)
        reward = head_sums(
            read_ref[:, at].astype(f32) * key_ref[:, at].astype(f32) * scales_ref[:, at]
        )
        merged[:, at] = (
            (normed + reward * value_ref[:, at].astype(f32)) * switch_ref[:, at].astype(f32)
        ).astype(bf16)
    out_ref[...] = jnp.dot(merged[...], matrix_ref[...], preferred_element_type=f32).astype(bf16)


def merge(place, local, coef, states, maps, read, key, value, switch, scales, matrix):
    length, breadth = local.shape
    pairs = breadth // PAIR
    rows = ROWS_OUT if length % ROWS_OUT == 0 else CHUNK
    wide = pl.BlockSpec((rows, breadth), lambda c: (c, 0))
    whole = pl.BlockSpec(states.shape, lambda c: (0, 0, 0, 0))
    return pl.pallas_call(
        merge_kernel,
        grid=(length // rows,),
        in_specs=[
            pl.BlockSpec(memory_space=pltpu.SMEM),
            wide, wide, whole, whole, wide, wide, wide, wide,
            pl.BlockSpec((1, breadth), lambda c: (0, 0)),
            pl.BlockSpec(matrix.shape, lambda c: (0, 0)),
        ],
        out_specs=pl.BlockSpec((rows, matrix.shape[1]), lambda c: (c, 0)),
        out_shape=jax.ShapeDtypeStruct((length, matrix.shape[1]), bf16),
        scratch_shapes=[pltpu.VMEM((pairs, PAIR, PAIR), f32), pltpu.VMEM((rows, breadth), bf16)],
        cost_estimate=pl.CostEstimate(
            flops=2 * length * breadth * matrix.shape[1],
            bytes_accessed=length * breadth * 14 + 2 * matrix.size + 2 * length * matrix.shape[1],
            transcendentals=0,
        ),
        name="merge",
    )(place, local, coef, states, maps, read, key, value, switch, scales[None, :], matrix)


def per_device(
    skip_stream,
    acceptance_signal,
    lookup_mapped,
    payload_mapped,
    result_switch,
    forget_dynamic_share,
    additive_forget_logarithm,
    forget_feature_offset,
    substitution_dynamic_share,
    substitution_feature_offset,
    diagonal_reward_scales,
    result_matrix,
    mlp_rescaler,
    switch_matrix,
    expand_matrix,
    contract_matrix,
):
    gate_whole, up_whole, down_whole = (
        lax.all_gather(switch_matrix, "sp", axis=0, tiled=True),
        lax.all_gather(expand_matrix, "sp", axis=0, tiled=True),
        lax.all_gather(contract_matrix, "sp", axis=0, tiled=True),
    )
    local, coef, state, move = recurrence(
        acceptance_signal,
        lookup_mapped,
        payload_mapped,
        forget_dynamic_share,
        additive_forget_logarithm,
        substitution_dynamic_share,
        forget_feature_offset,
        substitution_feature_offset,
    )
    states = lax.all_gather(state, "sp")
    maps = lax.all_gather(move, "sp")
    partial_rows = merge(
        lax.axis_index("sp").astype(jnp.int32)[None],
        local,
        coef,
        states,
        maps,
        acceptance_signal,
        lookup_mapped,
        payload_mapped,
        result_switch,
        diagonal_reward_scales,
        result_matrix,
    )
    projected = lax.psum_scatter(
        partial_rows,
        "tp",
        scatter_dimension=0,
        tiled=True,
    )
    stream = skip_stream.astype(jnp.float32) + lax.optimization_barrier(projected).astype(
        jnp.float32
    )
    scale_rows = lax.rsqrt(jnp.mean(stream * stream, axis=-1, keepdims=True) + norm_eps)
    normed_rows = (stream * scale_rows * mlp_rescaler[None, :]).astype(jnp.bfloat16)
    whole_rows = lax.all_gather(normed_rows, "tp", axis=0, tiled=True)
    gate_act = jnp.dot(whole_rows, gate_whole, preferred_element_type=jnp.float32)
    up_act = jnp.dot(whole_rows, up_whole, preferred_element_type=jnp.float32)
    hidden = (jax.nn.silu(gate_act) * up_act).astype(jnp.bfloat16)
    row_block = hidden
    ffn_out = lax.psum_scatter(
        lax.dot_general(
            row_block, down_whole, (((1,), (1,)), ((), ())), preferred_element_type=jnp.float32
        ).astype(jnp.bfloat16),
        "tp",
        scatter_dimension=0,
        tiled=True,
    )
    return (stream + half_step * lax.optimization_barrier(ffn_out).astype(jnp.float32)).astype(
        jnp.bfloat16
    )


def solution(mesh):
    placed = (
        P(("sp", "tp"), None),
        P("sp", "tp"),
        P("sp", "tp"),
        P("sp", "tp"),
        P("sp", "tp"),
        P("sp", "tp"),
        P("sp", "tp"),
        P("tp"),
        P("sp", "tp"),
        P("tp"),
        P("tp"),
        P("tp", None),
        P(),
        P("sp", "tp"),
        P("sp", "tp"),
        P("sp", "tp"),
    )
    return jax.shard_map(
        per_device, mesh=mesh, in_specs=placed, out_specs=P(("sp", "tp"), None), check_vma=False
    )
```

```python
import functools

import jax
import jax.numpy as jnp
from jax import lax
from jax.experimental import pallas as pl
from jax.experimental.pallas import tpu as pltpu
from jax.sharding import PartitionSpec as P

PER_GROUP_DIMS = 64


norm_eps = 1e-06
group_eps = 0.00064
half_step = 0.5
exact = lax.Precision.HIGHEST

PAIR = 2 * PER_GROUP_DIMS
CHUNK = 64
ROWS_OUT = 256
NT = (((1,), (1,)), ((), ()))
NN = (((1,), (0,)), ((), ()))
TN = (((0,), (0,)), ((), ()))
bf16 = jnp.bfloat16
f32 = jnp.float32
P_SCORE, P_INV, P_SOLVE, P_OUT, P_STATE = 3, 1, 3, 3, 1


def mm(left, right, dims, passes):
    if passes == 6:
        return lax.dot_general(left, right, dims, precision=exact, preferred_element_type=f32)
    left_hi, right_hi = left.astype(bf16), right.astype(bf16)
    total = lax.dot_general(left_hi, right_hi, dims, preferred_element_type=f32)
    if passes == 3:
        left_lo = (left - left_hi.astype(f32)).astype(bf16)
        right_lo = (right - right_hi.astype(f32)).astype(bf16)
        total += lax.dot_general(left_hi, right_lo, dims, preferred_element_type=f32)
        total += lax.dot_general(left_lo, right_hi, dims, preferred_element_type=f32)
    return total


def halves(shape):
    return lax.broadcasted_iota(jnp.int32, shape, 1) < PER_GROUP_DIMS


def stack(values):
    first = halves(values.shape)
    zero = jnp.zeros_like(values)
    return jnp.concatenate([jnp.where(first, values, zero), jnp.where(first, zero, values)], 0)


def fold(values):
    size = values.shape[0] // 2
    return values[:size] + values[size:]


def head_sums(values):
    row = lax.broadcasted_iota(jnp.int32, (PAIR, PAIR), 0) // PER_GROUP_DIMS
    col = lax.broadcasted_iota(jnp.int32, (PAIR, PAIR), 1) // PER_GROUP_DIMS
    ones = jnp.where(row == col, 1.0, 0.0).astype(bf16)
    hi = values.astype(bf16)
    left = values - hi.astype(f32)
    mid = left.astype(bf16)
    low = (left - mid.astype(f32)).astype(bf16)
    return (
        jnp.dot(hi, ones, preferred_element_type=f32)
        + jnp.dot(mid, ones, preferred_element_type=f32)
        + jnp.dot(low, ones, preferred_element_type=f32)
    )


def recur_kernel(
    read_ref, key_ref, value_ref, forget_ref, added_ref, rate_ref, forget_off_ref, rate_off_ref,
    out_ref, coef_ref, state_out_ref, map_out_ref, memory,
):
    pairs = read_ref.shape[1] // PAIR
    span = range(pairs)
    row = lax.broadcasted_iota(jnp.int32, (PAIR, PAIR), 0)
    col = lax.broadcasted_iota(jnp.int32, (PAIR, PAIR), 1)
    diagonal = jnp.where(row == col, 1.0, 0.0)
    same_head = (row // CHUNK) == (col // CHUNK)
    strict = same_head & (col < row)
    inclusive = same_head & (col <= row)

    @pl.when(pl.program_id(0) == 0)
    def _():
        for p in span:
            memory[p, :PAIR] = jnp.zeros((PAIR, PAIR), f32)
            memory[p, PAIR:] = diagonal

    lower = (
        lax.broadcasted_iota(jnp.int32, (CHUNK, CHUNK), 1)
        <= lax.broadcasted_iota(jnp.int32, (CHUNK, CHUNK), 0)
    )
    lower = jnp.where(lower, 1.0, 0.0)
    first = halves((CHUNK, PAIR))
    at = [slice(p * PAIR, (p + 1) * PAIR) for p in span]
    decay_rate = [
        jax.nn.sigmoid(forget_off_ref[:, at[p]] + forget_ref[:, at[p]].astype(f32)) for p in span
    ]
    log_step = [
        -0.6065306597126334 * decay_rate[p]
        + jnp.where(first, added_ref[:, 2 * p : 2 * p + 1], added_ref[:, 2 * p + 1 : 2 * p + 2])
        for p in span
    ]
    cumulate = [mm(lower, log_step[p], NN, 6) for p in span]
    key = [key_ref[:, at[p]].astype(f32) for p in span]
    unit = [key[p] * lax.rsqrt(head_sums(key[p] * key[p]) + norm_eps) for p in span]
    erase = [
        unit[p] * jax.nn.sigmoid(rate_off_ref[:, at[p]] + rate_ref[:, at[p]].astype(f32))
        for p in span
    ]
    middle = [cumulate[p][CHUNK // 2 - 1 : CHUNK // 2] for p in span]
    last = [cumulate[p][CHUNK - 1 : CHUNK] for p in span]
    growth = [jnp.exp(cumulate[p] - middle[p]) for p in span]
    shrink = [jnp.exp(middle[p] - cumulate[p]) for p in span]
    to_middle = [jnp.exp(middle[p]) for p in span]
    from_middle = [jnp.exp(last[p] - middle[p]) for p in span]
    over_chunk = [jnp.exp(last[p]) for p in span]
    before = [jnp.exp(cumulate[p] - log_step[p] - middle[p]) * unit[p] for p in span]
    read = [read_ref[:, at[p]].astype(f32) * growth[p] for p in span]
    key_back = [key[p] * shrink[p] for p in span]
    erase_back = [erase[p] * shrink[p] for p in span]
    score = [
        mm(
            jnp.concatenate([stack(before[p]), stack(read[p])], 0),
            jnp.concatenate([stack(key_back[p]), stack(erase_back[p])], 0),
            NT,
            P_SCORE,
        )
        for p in span
    ]
    key_past = [jnp.where(strict, score[p][:PAIR, :PAIR], 0.0) for p in span]
    erase_past = [jnp.where(strict, score[p][:PAIR, PAIR:], 0.0) for p in span]
    key_read = [jnp.where(inclusive, score[p][PAIR:, :PAIR], 0.0) for p in span]
    erase_read = [jnp.where(inclusive, score[p][PAIR:, PAIR:], 0.0) for p in span]
    value = [stack(value_ref[:, at[p]]).astype(f32) for p in span]
    recall = [mm(key_past[p], value[p], NN, P_SOLVE) for p in span]
    inverse = [
        diagonal - jnp.where((row // 2) == (col // 2), erase_past[p], 0.0) for p in span
    ]
    size = 2
    while size < CHUNK:
        off = ((row // (2 * size)) == (col // (2 * size))) & ((row // size) != (col // size))
        part = [mm(jnp.where(off, erase_past[p], 0.0), inverse[p], NN, P_INV) for p in span]
        inverse = [inverse[p] - mm(inverse[p], part[p], NN, P_INV) for p in span]
        size *= 2
    solved = [
        mm(
            inverse[p],
            jnp.concatenate([recall[p], stack(before[p] * to_middle[p])], 1),
            NN,
            P_SOLVE,
        )
        for p in span
    ]
    inner = [
        mm(
            jnp.concatenate([key_read[p], -erase_read[p]], 1),
            jnp.concatenate(
                [jnp.concatenate([value[p], jnp.zeros_like(value[p])], 1), solved[p]], 0
            ),
            NN,
            P_OUT,
        )
        for p in span
    ]
    local = [fold(inner[p][:, :PAIR]) for p in span]
    from_start = [fold(inner[p][:, PAIR:]) + read[p] * to_middle[p] for p in span]
    both = [memory[p] for p in span]
    passed = [mm(from_start[p], both[p], NT, P_STATE) for p in span]
    for p in span:
        out_ref[:, at[p]] = local[p] + passed[p][:, :PAIR]
        coef_ref[:, at[p]] = passed[p][:, PAIR:].astype(bf16)
    key_end = [key_back[p] * from_middle[p] for p in span]
    erase_end = [erase_back[p] * from_middle[p] for p in span]
    recalled = [fold(solved[p][:, :PAIR]) for p in span]
    carried_map = [fold(solved[p][:, PAIR:]) for p in span]
    added = [
        mm(
            jnp.concatenate([value_ref[:, at[p]].astype(f32), -recalled[p]], 0),
            jnp.concatenate([key_end[p], erase_end[p]], 0),
            TN,
            P_OUT,
        )
        for p in span
    ]
    step_map = [mm(carried_map[p], erase_end[p], TN, P_OUT) for p in span]
    for p in span:
        moved = mm(both[p], jnp.where(same_head, step_map[p], 0.0), NN, P_STATE)
        kept = both[p] * over_chunk[p] - moved
        memory[p, :PAIR] = kept[:PAIR] + jnp.where(same_head, added[p], 0.0)
        memory[p, PAIR:] = kept[PAIR:]

    @pl.when(pl.program_id(0) == pl.num_programs(0) - 1)
    def _():
        for p in span:
            state_out_ref[p] = fold(memory[p, :PAIR]).astype(bf16)
            map_out_ref[p] = fold(memory[p, PAIR:]).astype(bf16)


def recurrence(read, key, value, forget, added, rate, forget_off, rate_off):
    length, breadth = read.shape
    pairs = breadth // PAIR
    wide = pl.BlockSpec((CHUNK, breadth), lambda c: (c, 0))
    vector = pl.BlockSpec((1, breadth), lambda c: (0, 0))
    closing = pl.BlockSpec((pairs, PER_GROUP_DIMS, PAIR), lambda c: (0, 0, 0))
    closing_shape = jax.ShapeDtypeStruct((pairs, PER_GROUP_DIMS, PAIR), bf16)
    return pl.pallas_call(
        recur_kernel,
        grid=(length // CHUNK,),
        in_specs=[
            wide, wide, wide, wide,
            pl.BlockSpec((CHUNK, added.shape[1]), lambda c: (c, 0)),
            wide, vector, vector,
        ],
        out_specs=[wide, wide, closing, closing],
        out_shape=[
            jax.ShapeDtypeStruct((length, breadth), f32),
            jax.ShapeDtypeStruct((length, breadth), bf16),
            closing_shape,
            closing_shape,
        ],
        scratch_shapes=[pltpu.VMEM((pairs, 2 * PAIR, PAIR), f32)],
        cost_estimate=pl.CostEstimate(
            flops=length * breadth * 200000, bytes_accessed=length * breadth * 16, transcendentals=0
        ),
        name="recurrence",
    )(read, key, value, forget, added, rate, forget_off[None, :], rate_off[None, :])


def share_kernel(mine_ref, all_ref, own_sem, send_sem, recv_sem):
    me, n = lax.axis_index("sp"), all_ref.shape[0]
    barrier = pltpu.get_barrier_semaphore()
    for step in range(1, n):
        pl.semaphore_signal(
            barrier,
            inc=1,
            device_id={"sp": lax.rem(me + step, n)},
            device_id_type=pl.DeviceIdType.MESH,
        )
    pl.semaphore_wait(barrier, n - 1)
    copies = [
        pltpu.make_async_remote_copy(
            src_ref=mine_ref,
            dst_ref=all_ref.at[me],
            send_sem=send_sem.at[step - 1],
            recv_sem=recv_sem.at[step - 1],
            device_id={"sp": lax.rem(me + step, n)},
            device_id_type=pl.DeviceIdType.MESH,
        )
        for step in range(1, n)
    ]
    for copy in copies:
        copy.start()
    own = pltpu.make_async_copy(mine_ref, all_ref.at[me], own_sem)
    own.start()
    own.wait()
    for copy in copies:
        copy.wait()


def share(mine):
    n = lax.axis_size("sp")
    everyone = pl.pallas_call(
        share_kernel,
        in_specs=[pl.BlockSpec(memory_space=pltpu.VMEM)],
        out_specs=pl.BlockSpec(memory_space=pltpu.VMEM),
        out_shape=jax.ShapeDtypeStruct((n,) + mine.shape, mine.dtype),
        scratch_shapes=[
            pltpu.SemaphoreType.DMA,
            pltpu.SemaphoreType.DMA((n - 1,)),
            pltpu.SemaphoreType.DMA((n - 1,)),
        ],
        compiler_params=pltpu.CompilerParams(collective_id=0, has_side_effects=True),
        cost_estimate=pl.CostEstimate(flops=0, bytes_accessed=40000000, transcendentals=0),
        name="share",
    )(mine)
    return everyone[:, 0], everyone[:, 1]


def merge_kernel(
    place_ref, local_ref, coef_ref, states_ref, maps_ref, read_ref, key_ref, value_ref,
    switch_ref, scales_ref, matrix_ref, out_ref, carried, merged,
):
    pairs = local_ref.shape[1] // PAIR
    span = range(pairs)

    @pl.when(pl.program_id(0) == 0)
    def _():
        for p in span:
            carried[p] = jnp.zeros((PAIR, PAIR), f32)

        def one(turn, _):
            for p in span:
                carried[p] = mm(
                    carried[p], stack(maps_ref[turn, p].astype(f32)), NN, 3
                ) + stack(states_ref[turn, p].astype(f32))
            return 0

        lax.fori_loop(0, place_ref[0], one, 0)

    for p in span:
        at = slice(p * PAIR, (p + 1) * PAIR)
        outcome = local_ref[:, at] + mm(coef_ref[:, at].astype(f32), carried[p], NT, 1)
        centred = outcome - head_sums(outcome) * (1.0 / PER_GROUP_DIMS)
        spread = head_sums(centred * centred) * (1.0 / PER_GROUP_DIMS)
        normed = centred * lax.rsqrt(spread + group_eps)
        reward = head_sums(
            read_ref[:, at].astype(f32) * key_ref[:, at].astype(f32) * scales_ref[:, at]
        )
        merged[:, at] = (
            (normed + reward * value_ref[:, at].astype(f32)) * switch_ref[:, at].astype(f32)
        ).astype(bf16)
    out_ref[...] = jnp.dot(merged[...], matrix_ref[...], preferred_element_type=f32).astype(bf16)


def merge(place, local, coef, states, maps, read, key, value, switch, scales, matrix):
    length, breadth = local.shape
    pairs = breadth // PAIR
    rows = ROWS_OUT if length % ROWS_OUT == 0 else CHUNK
    wide = pl.BlockSpec((rows, breadth), lambda c: (c, 0))
    whole = pl.BlockSpec(states.shape, lambda c: (0, 0, 0, 0))
    return pl.pallas_call(
        merge_kernel,
        grid=(length // rows,),
        in_specs=[
            pl.BlockSpec(memory_space=pltpu.SMEM),
            wide, wide, whole, whole, wide, wide, wide, wide,
            pl.BlockSpec((1, breadth), lambda c: (0, 0)),
            pl.BlockSpec(matrix.shape, lambda c: (0, 0)),
        ],
        out_specs=pl.BlockSpec((rows, matrix.shape[1]), lambda c: (c, 0)),
        out_shape=jax.ShapeDtypeStruct((length, matrix.shape[1]), bf16),
        scratch_shapes=[pltpu.VMEM((pairs, PAIR, PAIR), f32), pltpu.VMEM((rows, breadth), bf16)],
        cost_estimate=pl.CostEstimate(
            flops=2 * length * breadth * matrix.shape[1],
            bytes_accessed=length * breadth * 14 + 2 * matrix.size + 2 * length * matrix.shape[1],
            transcendentals=0,
        ),
        name="merge",
    )(place, local, coef, states, maps, read, key, value, switch, scales[None, :], matrix)


def per_device(
    skip_stream,
    acceptance_signal,
    lookup_mapped,
    payload_mapped,
    result_switch,
    forget_dynamic_share,
    additive_forget_logarithm,
    forget_feature_offset,
    substitution_dynamic_share,
    substitution_feature_offset,
    diagonal_reward_scales,
    result_matrix,
    mlp_rescaler,
    switch_matrix,
    expand_matrix,
    contract_matrix,
):
    gate_whole, up_whole, down_whole = (
        lax.all_gather(switch_matrix, "sp", axis=0, tiled=True),
        lax.all_gather(expand_matrix, "sp", axis=0, tiled=True),
        lax.all_gather(contract_matrix, "sp", axis=0, tiled=True),
    )
    local, coef, state, move = recurrence(
        acceptance_signal,
        lookup_mapped,
        payload_mapped,
        forget_dynamic_share,
        additive_forget_logarithm,
        substitution_dynamic_share,
        forget_feature_offset,
        substitution_feature_offset,
    )
    states, maps = share(jnp.stack([state, move]))
    local, gate_whole = lax.optimization_barrier((local, gate_whole))
    partial_rows = merge(
        lax.axis_index("sp").astype(jnp.int32)[None],
        local,
        coef,
        states,
        maps,
        acceptance_signal,
        lookup_mapped,
        payload_mapped,
        result_switch,
        diagonal_reward_scales,
        result_matrix,
    )
    projected = lax.psum_scatter(
        partial_rows,
        "tp",
        scatter_dimension=0,
        tiled=True,
    )
    stream = skip_stream.astype(jnp.float32) + lax.optimization_barrier(projected).astype(
        jnp.float32
    )
    scale_rows = lax.rsqrt(jnp.mean(stream * stream, axis=-1, keepdims=True) + norm_eps)
    normed_rows = (stream * scale_rows * mlp_rescaler[None, :]).astype(jnp.bfloat16)
    normed_rows, up_whole = lax.optimization_barrier((normed_rows, up_whole))
    whole_rows = lax.all_gather(normed_rows, "tp", axis=0, tiled=True)
    gate_act = jnp.dot(whole_rows, gate_whole, preferred_element_type=jnp.float32)
    up_act = jnp.dot(whole_rows, up_whole, preferred_element_type=jnp.float32)
    hidden = (jax.nn.silu(gate_act) * up_act).astype(jnp.bfloat16)
    row_block = hidden
    ffn_out = lax.psum_scatter(
        lax.dot_general(
            row_block, down_whole, (((1,), (1,)), ((), ())), preferred_element_type=jnp.float32
        ).astype(jnp.bfloat16),
        "tp",
        scatter_dimension=0,
        tiled=True,
    )
    return (stream + half_step * lax.optimization_barrier(ffn_out).astype(jnp.float32)).astype(
        jnp.bfloat16
    )


def solution(mesh):
    placed = (
        P(("sp", "tp"), None),
        P("sp", "tp"),
        P("sp", "tp"),
        P("sp", "tp"),
        P("sp", "tp"),
        P("sp", "tp"),
        P("sp", "tp"),
        P("tp"),
        P("sp", "tp"),
        P("tp"),
        P("tp"),
        P("tp", None),
        P(),
        P("sp", "tp"),
        P("sp", "tp"),
        P("sp", "tp"),
    )
    return jax.shard_map(
        per_device, mesh=mesh, in_specs=placed, out_specs=P(("sp", "tp"), None), check_vma=False
    )
```
